256 devices in a mesh: grp: 2 (over y), fs: 16 (over z), tp: 8 (over x, core).
Axes of the slice: x: 4, y: 2, z: 16, core: 2. Of those that a mesh axis runs over, the one named last changes fastest.
The devices are a block of a 4x16x16 slice.
Arguments:
- tokens: bfloat16 [128, 128, 2048], P(('grp', 'fs'), None, 'tp'), parts along dimension 0, may hold values from -100 to 100
- mix_gain: float32 [2048], replicated, may hold values from 0.1 to 1.9
- gate_outer: bfloat16 [2048, 1024], P('fs', 'tp'), may hold values from -0.125 to 0.125
- gate_inner: bfloat16 [2048, 1024], P('fs', 'tp'), may hold values from -0.125 to 0.125
- value_weight: bfloat16 [2048, 1024], P('fs', 'tp'), may hold values from -0.125 to 0.125
- conv_taps: float32 [3, 1024], replicated, may hold values from -3 to 3
- mix_out: bfloat16 [1024, 2048], P('tp', 'fs'), may hold values from -0.25 to 0.25
- ffn_gain: float32 [2048], replicated, may hold values from 0.1 to 1.9
- ffn_gate: bfloat16 [2048, 5632], P('fs', 'tp'), may hold values from -0.125 to 0.125
- ffn_up: bfloat16 [2048, 5632], P('fs', 'tp'), may hold values from -0.125 to 0.125
- ffn_down: bfloat16 [5632, 2048], P('tp', 'fs'), may hold values from -0.109375 to 0.109375
- out_gain: float32 [2048], replicated, may hold values from 0.1 to 1.9
Outputs:
- layer_out: bfloat16 [128, 128, 2048], P(('grp', 'fs'), None, 'tp'), parts along dimension 0
The draws below stay inside these ranges and needn't reach their ends.
There are 2 independent parts, one for each index of `grp`. The reference program is written for one: setup_inputs(seed, part) draws one part's arguments, and reference() takes and returns one part's arrays. A program takes and returns all parts, laid end to end along the dimension named above; an argument that names none is the same for every part. Nothing has to cross between parts.
All inputs are finite; a program needn't handle non-finite values.
Results may differ from the reference program's by a relative error of at most 0.015.
Values may be sent and summed in bfloat16 or wider, within the bound.
No kernel may reach another device: no remote copies, remote signals or barrier semaphores. Data moves between devices by JAX's collectives and lax.ppermute only.
A program may use at most 64 MiB of HBM per device.

```python
import math
import jax
import jax.numpy as jnp
from jax import lax

D = 2048
CA = 1024
FF = 5632
TAPS = 3
LEN = 128
SEQS = 64
N_TP = 8


def draw_tokens(key, part):
    first_key, second_key = jax.random.split(jax.random.fold_in(key, 11), 2)
    ramp = jnp.exp(jnp.linspace(math.log(0.4), math.log(4.0), D)).astype(jnp.float32)
    rough = jax.random.uniform(second_key, (D,), jnp.float32, 0.6, 1.4)
    values = jax.random.normal(first_key, (SEQS, LEN, D), jnp.float32) * ramp * rough
    return jnp.clip(values, -100.0, 100.0).astype(jnp.bfloat16)


def with_spikes(drawn, own_key, source, target, parts, factor):
    owner, partner = [(jnp.arange(drawn.shape[dim]) // (drawn.shape[dim] // parts)).reshape([-1 if axis == dim else 1 for axis in range(drawn.ndim)]) for dim in (source, target)]
    chosen = jax.random.permutation(own_key, parts)[partner]
    strong = (owner == chosen) | (owner == (partner + parts // 2) % parts)
    return jnp.where(strong, factor * drawn, drawn)


def block_levels(stream_key, dims, cuts, low, largest):
    factor_of, own = 1.0, jax.random.fold_in(stream_key, 6)
    for axis_at, shards_of in cuts:
        draws = jnp.exp(jax.random.uniform(jax.random.fold_in(own, axis_at), (shards_of,), jnp.float32, low / len(cuts), largest / len(cuts)))
        factor_of = factor_of * jnp.repeat(draws, dims[axis_at] // shards_of).reshape([-1 if axis == axis_at else 1 for axis in range(len(dims))])
    return factor_of


def centred(own_key, dims, spread, limit, cuts=(), held_as=jnp.bfloat16):
    values = spread * jax.random.normal(own_key, dims, jnp.float32)
    if cuts:
        values = values * block_levels(own_key, dims, cuts, -0.22, 0.18)
    return jnp.clip(values, -limit, limit).astype(held_as)


def gaussian_with(key, extent, scale, limit, pieces, heavy, held_as=jnp.bfloat16):
    result = scale * jax.random.normal(key, extent, jnp.float32)
    if pieces:
        result = result * block_levels(key, extent, pieces, -0.22, 0.18)
    return jnp.clip(with_spikes(result, jax.random.fold_in(key, 3), *heavy), -limit, limit).astype(held_as)


def setup_inputs(seed: int = 0, part: int = 0) -> dict:
    streams_of = jax.random.split(jax.random.key(seed), 13)
    part_splits = jax.random.split(jax.random.fold_in(streams_of[12], part), 13)
    return {
        "tokens": draw_tokens(jax.random.fold_in(jax.random.fold_in(streams_of[12], part), 71), part),
        "mix_gain": jnp.clip(1.0 + 0.18 * jax.random.normal(streams_of[1], (D,), jnp.float32), 0.1, 1.9),
        "gate_outer": centred(streams_of[2], (D, CA), D ** -0.5, 0.125, ((0, 16), (1, 8))),
        "gate_inner": centred(streams_of[3], (D, CA), D ** -0.5, 0.125, ((0, 16), (1, 8))),
        "value_weight": centred(streams_of[4], (D, CA), D ** -0.5, 0.125, ((0, 16), (1, 8))),
        "conv_taps": centred(streams_of[5], (TAPS, CA), 0.6, 3.0, (), jnp.float32),
        "mix_out": gaussian_with(streams_of[6], (CA, D), CA ** -0.5, 0.25, ((0, 8), (1, 16)), (0, 1, 16, 2.0)),
        "ffn_gain": jnp.clip(1.0 + 0.18 * jax.random.normal(streams_of[7], (D,), jnp.float32), 0.1, 1.9),
        "ffn_gate": centred(streams_of[8], (D, FF), D ** -0.5, 0.125, ((0, 16), (1, 8))),
        "ffn_up": centred(streams_of[9], (D, FF), D ** -0.5, 0.125, ((0, 16), (1, 8))),
        "ffn_down": gaussian_with(streams_of[10], (FF, D), FF ** -0.5, 0.109375, ((0, 8), (1, 16)), (0, 1, 16, 2.0)),
        "out_gain": jnp.clip(1.0 + 0.18 * jax.random.normal(streams_of[11], (D,), jnp.float32), 0.1, 1.9),
    }


def rms_norm(values, gain):
    floats = values.astype(jnp.float32)
    scaled = floats * lax.rsqrt(lax.optimization_barrier(jnp.mean(floats * floats, axis=-1, keepdims=True)) + 1e-06)
    return scaled * gain.astype(jnp.float32)

def blocked_sum(left, weight, blocks):
    width = left.shape[1] // blocks
    summed = jnp.zeros((left.shape[0], weight.shape[1]), jnp.float32)
    for number in range(blocks):
        partial_value = jnp.dot(left[:, number * width:(number + 1) * width], weight[number * width:(number + 1) * width], preferred_element_type=jnp.float32).astype(jnp.bfloat16)
        summed = summed + lax.optimization_barrier(partial_value).astype(jnp.float32)
    return summed

def reference(tokens, mix_gain, gate_outer, gate_inner, value_weight, conv_taps, mix_out, ffn_gain, ffn_gate, ffn_up, ffn_down, out_gain):
    rows = SEQS * LEN
    flat = tokens.reshape(rows, D)
    normed = rms_norm(flat, mix_gain).astype(jnp.bfloat16)
    outer = jnp.dot(normed, gate_outer, preferred_element_type=jnp.float32).astype(jnp.bfloat16)
    inner = jnp.dot(normed, gate_inner, preferred_element_type=jnp.float32).astype(jnp.bfloat16)
    values = jnp.dot(normed, value_weight, preferred_element_type=jnp.float32).astype(jnp.bfloat16)
    product = (inner.astype(jnp.float32) * values.astype(jnp.float32)).reshape(SEQS, LEN, CA)
    padded = jnp.pad(product, ((0, 0), (TAPS - 1, 0), (0, 0)))
    conv = jnp.zeros((SEQS, LEN, CA), jnp.float32)
    for offset in range(TAPS):
        conv = conv + conv_taps[offset].astype(jnp.float32) * padded[:, offset:offset + LEN]
    gated = (outer.astype(jnp.float32) * conv.reshape(rows, CA)).astype(jnp.bfloat16)
    first = (flat.astype(jnp.float32) + blocked_sum(gated, mix_out, N_TP)).astype(jnp.bfloat16)
    normed_ffn = rms_norm(first, ffn_gain).astype(jnp.bfloat16)
    gate = jnp.dot(normed_ffn, ffn_gate, preferred_element_type=jnp.float32)
    upward = jnp.dot(normed_ffn, ffn_up, preferred_element_type=jnp.float32)
    hidden = (jax.nn.silu(gate) * upward).astype(jnp.bfloat16)
    second = first.astype(jnp.float32) + blocked_sum(hidden, ffn_down, N_TP)
    return rms_norm(second, out_gain).astype(jnp.bfloat16).reshape(SEQS, LEN, D)
```

```python
import functools
import jax
import jax.numpy as jnp
from jax import lax
from jax.experimental import pallas as pl
from jax.experimental.pallas import tpu as pltpu
from jax.sharding import PartitionSpec as P

F32 = jnp.float32
BF16 = jnp.bfloat16


def shift(v, axis, by):
    n = lax.axis_size(axis)
    return lax.ppermute(v, axis, [(a, (a + by) % n) for a in range(n)])


def swap(v, axis):
    n = lax.axis_size(axis)
    return lax.ppermute(v, axis, [(a, a ^ 1) for a in range(n)])


def ring_offsets(n):
    pairs = [(0, n // 2)]
    for s in range(1, n // 2):
        pairs.append((n - s, s))
    return pairs


def ring(v, axis):
    n = lax.axis_size(axis)
    slots = {0: v}
    f = b = v
    for s in range(1, n // 2 + 1):
        f = shift(f, axis, 1)
        slots[n - s] = f
        if s < n // 2:
            b = shift(b, axis, -1)
            slots[s] = b
    return slots


def gather_rows(v):
    own = [v, shift(v, "tp", -2), shift(v, "tp", 4), shift(v, "tp", 2)]
    return own + [swap(a, "tp") for a in own]


def block_of(t, slot, n):
    base = t if slot < n // 2 else t ^ 1
    return (base + 2 * (slot % (n // 2))) % n


def scatter_sum(parts, base):
    keep, give = parts
    n = len(keep)
    got = [swap(g, "tp") for g in give]
    sums = [k.astype(F32) + g.astype(F32) for k, g in zip(keep, got)]
    total = base.astype(F32) + sums[0]
    for d in range(1, n):
        total = total + shift(sums[d].astype(BF16), "tp", 2 * d).astype(F32)
    return total


def normalize(t, blocks, gain_ref, xn_ref, rows=128):
    count = len(blocks)
    cols = blocks[0].shape[1]
    half = xn_ref.shape[2]
    for r in range(0, blocks[0].shape[0], rows):
        sl = pl.ds(r, rows)
        acc = jnp.zeros((rows, 1), F32)
        for ref in blocks:
            v = ref[sl, :].astype(F32)
            acc = acc + jnp.sum(v * v, axis=1, keepdims=True)
        scale = lax.rsqrt(acc / (count * cols) + 1e-06)
        for slot, ref in enumerate(blocks):
            b = block_of(t, slot, count)
            v = ref[sl, :].astype(F32) * scale
            for h in range(cols // half):
                k = b * (cols // half) + h
                g = gain_ref[pl.ds(k, 1), :]
                xn_ref[k, sl, :] = (v[:, h * half : (h + 1) * half] * g).astype(BF16)


def mixer_body(*refs, n_blocks, n_slots, channels, length):
    blocks = refs[:n_blocks]
    slots = refs[n_blocks : n_blocks + n_slots]
    gain_ref, taps_ref = refs[n_blocks + n_slots : n_blocks + n_slots + 2]
    outs = refs[n_blocks + n_slots + 2 : n_blocks + n_slots + 2 + n_blocks]
    xn_ref, o_ref = refs[-2:]
    t = lax.axis_index("tp")
    i = lax.axis_index("fs")
    normalize(t, blocks, gain_ref, xn_ref)
    pairs = ring_offsets(n_slots)
    acc = None
    for n, (a, b) in enumerate(pairs):
        ka, kb = (i + a) % n_slots, (i + b) % n_slots
        wa, wb = slots[2 * n], slots[2 * n + 1]
        lhs = jnp.concatenate([xn_ref[ka], xn_ref[kb]], axis=1)
        rhs = jnp.concatenate([wa[:, : 3 * channels], wb[:, : 3 * channels]], axis=0)
        part = jnp.dot(lhs, rhs, preferred_element_type=F32)
        acc = part if acc is None else acc + part
        o_ref[ka] = wa[:, 3 * channels :]
        o_ref[kb] = wb[:, 3 * channels :]
    acc = acc.astype(BF16).astype(F32)
    outer, inner, values = (acc[:, q * channels : (q + 1) * channels] for q in range(3))
    product = inner * values
    at = lax.broadcasted_iota(jnp.int32, product.shape, 0) % length
    tap_count = taps_ref.shape[0]
    conv = jnp.zeros(product.shape, F32)
    for q in range(tap_count):
        back = tap_count - 1 - q
        moved = product
        if back:
            moved = jnp.where(at >= back, pltpu.roll(product, back, 0), 0.0)
        conv = conv + taps_ref[pl.ds(q, 1), pl.ds(pl.multiple_of(t * channels, channels), channels)] * moved
    gated = (outer * conv).astype(BF16)
    send_parts(t, gated, o_ref, outs)


def send_parts(t, left, w_ref, outs):
    n = len(outs)
    per = w_ref.shape[0] // n
    for slot in range(n):
        b = block_of(t, slot, n)
        rhs = jnp.concatenate([w_ref[b * per + h] for h in range(per)], axis=1)
        outs[slot][...] = jnp.dot(left, rhs, preferred_element_type=F32).astype(BF16)


def hidden_body(*refs, n_blocks, n_slots):
    at = 0
    blocks = refs[:n_blocks]
    at = n_blocks
    own, other, down = (refs[at + q * n_slots : at + (q + 1) * n_slots] for q in range(3))
    at += 3 * n_slots
    gain_ref = refs[at]
    outs = refs[at + 1 : at + 1 + n_blocks]
    xn_ref, d_ref = refs[-2:]
    t = lax.axis_index("tp")
    i = lax.axis_index("fs")
    p = lax.axis_index("grp") % 2
    normalize(t, blocks, gain_ref, xn_ref)
    pairs = ring_offsets(n_slots)
    sums = [None, None]
    for n, (a, b) in enumerate(pairs):
        ka, kb = (i + a) % n_slots, (i + b) % n_slots
        lhs = jnp.concatenate([xn_ref[ka], xn_ref[kb]], axis=1)
        for q, w in enumerate((own, other)):
            rhs = jnp.concatenate([w[2 * n][...], w[2 * n + 1][...]], axis=0)
            part = jnp.dot(lhs, rhs, preferred_element_type=F32)
            sums[q] = part if sums[q] is None else sums[q] + part
        d_ref[ka] = down[2 * n][...]
        d_ref[kb] = down[2 * n + 1][...]
    gate = jnp.where(p == 0, sums[0], sums[1])
    upward = jnp.where(p == 0, sums[1], sums[0])
    hidden = (gate / (1.0 + jnp.exp(-gate)) * upward).astype(BF16)
    send_parts(t, hidden, d_ref, outs)


def run_kernel(body, args, out_shape, scratch, name, flops, **static):
    return pl.pallas_call(
        functools.partial(body, **static),
        out_shape=out_shape,
        in_specs=[pl.BlockSpec(memory_space=pltpu.VMEM)] * len(args),
        out_specs=[pl.BlockSpec(memory_space=pltpu.VMEM)] * len(out_shape),
        scratch_shapes=scratch,
        compiler_params=pltpu.CompilerParams(vmem_limit_bytes=40 * 1024 * 1024),
        cost_estimate=pl.CostEstimate(flops=flops, transcendentals=0, bytes_accessed=1 << 20),
        name=name,
    )(*args)


def local(
    tokens,
    mix_gain,
    gate_outer,
    gate_inner,
    value_weight,
    conv_taps,
    mix_out,
    ffn_gain,
    ffn_gate,
    ffn_up,
    ffn_down,
    out_gain,
):
    seq_count, length, columns = tokens.shape
    row_count = seq_count * length
    n_tp = lax.axis_size("tp")
    n_fs = lax.axis_size("fs")
    width = columns * n_tp
    channels = gate_outer.shape[1]
    units = ffn_gate.shape[1]
    kdim = gate_outer.shape[0]
    mine = tokens.reshape(row_count, columns)
    p = lax.axis_index("grp") % 2
    order = [o for pair in ring_offsets(n_fs) for o in pair]

    mixer_w = jnp.concatenate([gate_outer, gate_inner, value_weight, mix_out], axis=1)
    mixer_slots = ring(mixer_w, "fs")
    blocks = gather_rows(mine)
    own_w = jnp.where(p == 0, ffn_gate, ffn_up)
    own_slots = ring(own_w, "fs")
    other_slots = {o: swap(own_slots[o], "grp") for o in order}
    down_slots = ring(ffn_down, "fs")

    part = jax.ShapeDtypeStruct((row_count, columns), BF16)
    xn = pltpu.VMEM((n_fs, row_count, kdim), BF16)
    parts = run_kernel(
        mixer_body,
        blocks + [mixer_slots[o] for o in order] + [mix_gain.reshape(n_fs, kdim), conv_taps],
        [part] * n_tp,
        [xn, pltpu.VMEM((n_fs, channels, kdim), BF16)],
        "mixer",
        2 * row_count * width * 4 * channels,
        n_blocks=n_tp,
        n_slots=n_fs,
        channels=channels,
        length=length,
    )
    first = scatter_sum((parts[: n_tp // 2], parts[n_tp // 2 :]), mine).astype(BF16)
    blocks = gather_rows(first)
    parts = run_kernel(
        hidden_body,
        blocks
        + [own_slots[o] for o in order]
        + [other_slots[o] for o in order]
        + [down_slots[o] for o in order]
        + [ffn_gain.reshape(n_fs, kdim)],
        [part] * n_tp,
        [xn, pltpu.VMEM((n_fs, units, kdim), BF16)],
        "ffn",
        2 * row_count * width * 3 * units,
        n_blocks=n_tp,
        n_slots=n_fs,
    )
    second = scatter_sum((parts[: n_tp // 2], parts[n_tp // 2 :]), first)
    squares = jnp.sum(second * second, axis=1).reshape(row_count // 128, 128)
    squares = squares + swap(squares, "tp")
    squares = squares + shift(squares, "tp", 2) + shift(squares, "tp", 4) + shift(squares, "tp", 6)
    factor = lax.rsqrt(squares.reshape(row_count) / width + 1e-06)
    own_gain = lax.dynamic_slice_in_dim(out_gain, lax.axis_index("tp") * columns, columns, 0)
    result = second * factor[:, None] * own_gain
    return result.astype(BF16).reshape(seq_count, length, columns)


def solution(mesh):
    in_specs = (
        P(("grp", "fs"), None, "tp"),
        P(),
        P("fs", "tp"),
        P("fs", "tp"),
        P("fs", "tp"),
        P(),
        P("tp", "fs"),
        P(),
        P("fs", "tp"),
        P("fs", "tp"),
        P("tp", "fs"),
        P(),
    )
    out_specs = P(("grp", "fs"), None, "tp")
    return jax.shard_map(local, mesh=mesh, in_specs=in_specs, out_specs=out_specs, check_vma=False)
```

```python
import functools
import jax
import jax.numpy as jnp
from jax import lax
from jax.experimental import pallas as pl
from jax.experimental.pallas import tpu as pltpu
from jax.sharding import PartitionSpec as P

F32 = jnp.float32
BF16 = jnp.bfloat16


def shift(v, axis, by):
    n = lax.axis_size(axis)
    return lax.ppermute(v, axis, [(a, (a + by) % n) for a in range(n)])


def swap(v, axis):
    n = lax.axis_size(axis)
    return lax.ppermute(v, axis, [(a, a ^ 1) for a in range(n)])


def ring_offsets(n):
    pairs = [(0, n // 2)]
    for s in range(1, n // 2):
        pairs.append((n - s, s))
    return pairs


def ring(v, axis):
    n = lax.axis_size(axis)
    slots = {0: v}
    f = b = v
    for s in range(1, n // 2 + 1):
        f = shift(f, axis, 1)
        slots[n - s] = f
        if s < n // 2:
            b = shift(b, axis, -1)
            slots[s] = b
    return slots


def gather_rows(v):
    own = [v, shift(v, "tp", -2), shift(v, "tp", 4), shift(v, "tp", 2)]
    return own + [swap(a, "tp") for a in own]


def block_of(t, slot, n):
    base = t if slot < n // 2 else t ^ 1
    return (base + 2 * (slot % (n // 2))) % n


def scatter_sum(parts, base):
    keep, give = parts
    n = len(keep)
    got = [swap(g, "tp") for g in give]
    sums = [k.astype(F32) + g.astype(F32) for k, g in zip(keep, got)]
    total = base.astype(F32) + sums[0]
    for d in range(1, n):
        total = total + shift(sums[d].astype(BF16), "tp", 2 * d).astype(F32)
    return total


def normalize(t, blocks, gain_ref, xn_ref, rows=128):
    count = len(blocks)
    cols = blocks[0].shape[1]
    half = xn_ref.shape[2]

    @pl.loop(0, blocks[0].shape[0] // rows)
    def _(r):
        sl = pl.ds(pl.multiple_of(r * rows, rows), rows)
        acc = jnp.zeros((rows, 1), F32)
        for ref in blocks:
            v = ref[sl, :].astype(F32)
            acc = acc + jnp.sum(v * v, axis=1, keepdims=True)
        scale = lax.rsqrt(acc / (count * cols) + 1e-06)
        for slot, ref in enumerate(blocks):
            b = block_of(t, slot, count)
            v = ref[sl, :].astype(F32) * scale
            for h in range(cols // half):
                k = b * (cols // half) + h
                g = gain_ref[pl.ds(k, 1), :]
                xn_ref[k, sl, :] = (v[:, h * half : (h + 1) * half] * g).astype(BF16)


def pack_body(*refs):
    mats, (gate, up, down) = refs[:4], refs[4:7]
    mixer_ref, ffn_ref, flip_ref, ffn_buf, sems = refs[7:]
    units, kdim = gate.shape
    tiles = units // kdim
    lead = (2 * tiles + 1) * kdim
    moves = [(w, mixer_ref.at[q]) for q, w in enumerate(mats)]
    moves += [(gate, flip_ref.at[0]), (up, flip_ref.at[1]), (down, ffn_buf.at[pl.ds(lead, units)])]
    moves = [pltpu.make_async_copy(x, y, sems.at[n]) for n, (x, y) in enumerate(moves)]
    for c in moves:
        c.start()
    for c in moves:
        c.wait()
    for q in range(2):
        for j in range(tiles):
            ffn_buf[pl.ds((q * tiles + j) * kdim, kdim), :] = flip_ref[q, pl.ds(j * kdim, kdim), :].T
    rest = pl.ds(tiles * kdim, units - tiles * kdim)
    ends = jnp.concatenate([flip_ref[0, rest, :], flip_ref[1, rest, :]], axis=0)
    ffn_buf[pl.ds(2 * tiles * kdim, kdim), :] = ends.T
    last = pltpu.make_async_copy(ffn_buf, ffn_ref, sems.at[len(moves)])
    last.start()
    last.wait()


def norm_body(*refs, n_blocks):
    blocks, gain_ref, xn_ref = refs[:n_blocks], refs[n_blocks], refs[n_blocks + 1]
    normalize(lax.axis_index("tp"), blocks, gain_ref, xn_ref)


def mixer_body(*refs, n_slots, channels, length):
    xn_ref, taps_ref = refs[:2]
    slots = refs[2 : 2 + n_slots]
    outs, o_ref = refs[2 + n_slots : -1], refs[-1]
    t = lax.axis_index("tp")
    i = lax.axis_index("fs")
    pairs = ring_offsets(n_slots)
    for slot, off in zip(slots, [o for pair in pairs for o in pair]):
        o_ref[(i + off) % n_slots] = slot[3]
    rows = 2 * length

    @pl.loop(0, xn_ref.shape[1] // rows)
    def _(r):
        sl = pl.ds(pl.multiple_of(r * rows, rows), rows)
        acc = None
        for n, (a, b) in enumerate(pairs):
            ka, kb = (i + a) % n_slots, (i + b) % n_slots
            wa, wb = slots[2 * n], slots[2 * n + 1]
            lhs = jnp.concatenate([xn_ref[ka, sl, :], xn_ref[kb, sl, :]], axis=1)
            rhs = jnp.concatenate(
                [jnp.concatenate([w[q] for q in range(3)], axis=1) for w in (wa, wb)], axis=0
            )
            part = jnp.dot(lhs, rhs, preferred_element_type=F32)
            acc = part if acc is None else acc + part
        acc = acc.astype(BF16).astype(F32)
        outer, inner, values = (acc[:, q * channels : (q + 1) * channels] for q in range(3))
        product = inner * values
        at = lax.broadcasted_iota(jnp.int32, product.shape, 0) % length
        tap_count = taps_ref.shape[0]
        conv = jnp.zeros(product.shape, F32)
        for q in range(tap_count):
            back = tap_count - 1 - q
            moved = product
            if back:
                moved = jnp.where(at >= back, pltpu.roll(product, back, 0), 0.0)
            lanes = pl.ds(pl.multiple_of(t * channels, channels), channels)
            conv = conv + taps_ref[pl.ds(q, 1), lanes] * moved
        gated = (outer * conv).astype(BF16)
        send_parts(t, gated, lambda k: o_ref[k], n_slots, outs, sl)


def send_parts(t, left, weight, n_slots, outs, sl):
    n = len(outs)
    per = n_slots // n
    for slot in range(n):
        b = block_of(t, slot, n)
        rhs = jnp.concatenate([weight(b * per + h) for h in range(per)], axis=1)
        outs[slot][sl, :] = jnp.dot(left, rhs, preferred_element_type=F32).astype(BF16)


def hidden_body(xn_ref, w_hbm, *refs, units):
    outs = refs[:-3]
    w_ref, acc_ref, sems = refs[-3:]
    t = lax.axis_index("tp")
    n_slots, _, lanes = w_ref.shape
    kdim = xn_ref.shape[2]
    tiles = units // lanes
    pairs = n_slots // 2

    def fetch(n):
        return pltpu.make_async_copy(w_hbm.at[pl.ds(2 * n, 2)], w_ref.at[pl.ds(2 * n, 2)], sems.at[n])

    for n in range(pairs):
        fetch(n).start()
    acc_ref[...] = jnp.zeros(acc_ref.shape, F32)

    @pl.loop(0, pairs)
    def _(n):
        fetch(n).wait()
        lhs = jnp.concatenate([xn_ref[2 * n], xn_ref[2 * n + 1]], axis=1)
        rhs = jnp.concatenate(
            [
                jnp.concatenate([w_ref[2 * n + h, pl.ds(j * kdim, kdim), :] for j in range(2 * tiles + 1)], axis=1)
                for h in range(2)
            ],
            axis=0,
        )
        acc_ref[...] += jnp.dot(lhs, rhs, preferred_element_type=F32)

    full = tiles * lanes
    rest = units - full
    ends = acc_ref[:, 2 * full :]
    pieces = ((acc_ref[:, :full], acc_ref[:, full : 2 * full]), (ends[:, :rest], ends[:, rest:]))
    hidden = jnp.concatenate([(g / (1.0 + jnp.exp(-g)) * u).astype(BF16) for g, u in pieces], axis=1)
    down = pl.ds((2 * tiles + 1) * kdim, units)
    send_parts(t, hidden, lambda k: w_ref[k, down, :], n_slots, outs, slice(None))


def run_kernel(body, args, out_shape, scratch, name, flops, vmem=24, hbm=(), hbm_out=(), **static):
    def spec(far):
        return pl.BlockSpec(memory_space=pltpu.HBM if far else pltpu.VMEM)

    return pl.pallas_call(
        functools.partial(body, **static),
        out_shape=out_shape,
        in_specs=[spec(n in hbm) for n in range(len(args))],
        out_specs=[spec(n in hbm_out) for n in range(len(out_shape))],
        scratch_shapes=scratch,
        compiler_params=pltpu.CompilerParams(vmem_limit_bytes=vmem * 1024 * 1024),
        cost_estimate=pl.CostEstimate(flops=flops, transcendentals=0, bytes_accessed=1 << 20),
        name=name,
    )(*args)


def local(
    tokens,
    mix_gain,
    gate_outer,
    gate_inner,
    value_weight,
    conv_taps,
    mix_out,
    ffn_gain,
    ffn_gate,
    ffn_up,
    ffn_down,
    out_gain,
):
    seq_count, length, columns = tokens.shape
    row_count = seq_count * length
    n_tp = lax.axis_size("tp")
    n_fs = lax.axis_size("fs")
    width = columns * n_tp
    channels = gate_outer.shape[1]
    units = ffn_gate.shape[1]
    kdim = gate_outer.shape[0]
    mine = tokens.reshape(row_count, columns)
    order = [o for pair in ring_offsets(n_fs) for o in pair]

    mixer_w, ffn_w = run_kernel(
        pack_body,
        [gate_outer, gate_inner, value_weight, mix_out, ffn_gate.T, ffn_up.T, ffn_down],
        [
            jax.ShapeDtypeStruct((4, kdim, channels), BF16),
            jax.ShapeDtypeStruct((3 * units, kdim), BF16),
        ],
        [
            pltpu.VMEM((2, units, kdim), BF16),
            pltpu.VMEM((3 * units, kdim), BF16),
            pltpu.SemaphoreType.DMA((8,)),
        ],
        "pack",
        1 << 20,
        vmem=62,
        hbm=range(7),
        hbm_out=(1,),
    )
    ffn_all = lax.all_gather(ffn_w, "fs", axis=0, tiled=False)
    mixer_slots = ring(mixer_w, "fs")
    blocks = gather_rows(mine)

    part = jax.ShapeDtypeStruct((row_count, columns), BF16)
    xn = jax.ShapeDtypeStruct((n_fs, row_count, kdim), BF16)
    gains = (mix_gain.reshape(n_fs, kdim), ffn_gain.reshape(n_fs, kdim))
    (normed,) = run_kernel(norm_body, blocks + [gains[0]], [xn], [], "norm_mix", 1 << 30, n_blocks=n_tp)
    parts = run_kernel(
        mixer_body,
        [normed, conv_taps] + [mixer_slots[o] for o in order],
        [part] * n_tp,
        [pltpu.VMEM((n_fs, channels, kdim), BF16)],
        "mixer",
        2 * row_count * width * 4 * channels,
        n_slots=n_fs,
        channels=channels,
        length=length,
    )
    first = scatter_sum((parts[: n_tp // 2], parts[n_tp // 2 :]), mine).astype(BF16)
    blocks = gather_rows(first)
    (normed,) = run_kernel(norm_body, blocks + [gains[1]], [xn], [], "norm_ffn", 1 << 30, n_blocks=n_tp)
    parts = run_kernel(
        hidden_body,
        [normed, ffn_all],
        [part] * n_tp,
        [
            pltpu.VMEM(ffn_all.shape, BF16),
            pltpu.VMEM((row_count, 2 * units), F32),
            pltpu.SemaphoreType.DMA((n_fs // 2,)),
        ],
        "ffn",
        2 * row_count * width * 3 * units,
        vmem=52,
        hbm=(1,),
        units=units,
    )
    second = scatter_sum((parts[: n_tp // 2], parts[n_tp // 2 :]), first)
    squares = jnp.sum(second * second, axis=1)
    copies = jnp.broadcast_to(squares, (n_tp, row_count))
    squares = lax.all_to_all(copies, "tp", split_axis=0, concat_axis=0, tiled=True).sum(axis=0)
    factor = lax.rsqrt(squares.reshape(row_count) / width + 1e-06)
    own_gain = lax.dynamic_slice_in_dim(out_gain, lax.axis_index("tp") * columns, columns, 0)
    result = second * factor[:, None] * own_gain
    return result.astype(BF16).reshape(seq_count, length, columns)


def solution(mesh):
    in_specs = (
        P(("grp", "fs"), None, "tp"),
        P(),
        P("fs", "tp"),
        P("fs", "tp"),
        P("fs", "tp"),
        P(),
        P("tp", "fs"),
        P(),
        P("fs", "tp"),
        P("fs", "tp"),
        P("tp", "fs"),
        P(),
    )
    out_specs = P(("grp", "fs"), None, "tp")
    return jax.shard_map(local, mesh=mesh, in_specs=in_specs, out_specs=out_specs, check_vma=False)
```

```python
import functools
import jax
import jax.numpy as jnp
from jax import lax
from jax.experimental import pallas as pl
from jax.experimental.pallas import tpu as pltpu
from jax.sharding import PartitionSpec as P

F32 = jnp.float32
BF16 = jnp.bfloat16


def shift(v, axis, by):
    n = lax.axis_size(axis)
    return lax.ppermute(v, axis, [(a, (a + by) % n) for a in range(n)])


def swap(v, axis):
    n = lax.axis_size(axis)
    return lax.ppermute(v, axis, [(a, a ^ 1) for a in range(n)])


def ring_offsets(n):
    pairs = [(0, n // 2)]
    for s in range(1, n // 2):
        pairs.append((n - s, s))
    return pairs


def ring(v, axis):
    n = lax.axis_size(axis)
    slots = {0: v}
    f = b = v
    for s in range(1, n // 2 + 1):
        f = shift(f, axis, 1)
        slots[n - s] = f
        if s < n // 2:
            b = shift(b, axis, -1)
            slots[s] = b
    return slots


def gather_rows(v):
    own = [v, shift(v, "tp", -2), shift(v, "tp", 4), shift(v, "tp", 2)]
    return own + [swap(a, "tp") for a in own]


def block_of(t, slot, n):
    base = t if slot < n // 2 else t ^ 1
    return (base + 2 * (slot % (n // 2))) % n


def scatter_sum(parts, base):
    keep, give = parts
    n = len(keep)
    got = [swap(g, "tp") for g in give]
    sums = [k.astype(F32) + g.astype(F32) for k, g in zip(keep, got)]
    total = base.astype(F32) + sums[0]
    for d in range(1, n):
        total = total + shift(sums[d].astype(BF16), "tp", 2 * d).astype(F32)
    return total


def normalize(t, blocks, gain_ref, xn_ref, rows=128):
    count = len(blocks)
    cols = blocks[0].shape[1]
    half = xn_ref.shape[2]

    @pl.loop(0, blocks[0].shape[0] // rows)
    def _(r):
        sl = pl.ds(pl.multiple_of(r * rows, rows), rows)
        acc = jnp.zeros((rows, 1), F32)
        for ref in blocks:
            v = ref[sl, :].astype(F32)
            acc = acc + jnp.sum(v * v, axis=1, keepdims=True)
        scale = lax.rsqrt(acc / (count * cols) + 1e-06)
        for slot, ref in enumerate(blocks):
            b = block_of(t, slot, count)
            v = ref[sl, :].astype(F32) * scale
            for h in range(cols // half):
                k = b * (cols // half) + h
                g = gain_ref[pl.ds(k, 1), :]
                xn_ref[k, sl, :] = (v[:, h * half : (h + 1) * half] * g).astype(BF16)


def pack_body(*refs):
    mats, (gate, up, down) = refs[:4], refs[4:7]
    mixer_ref, ffn_ref, flip_ref, ffn_buf, sems = refs[7:]
    units, kdim = gate.shape
    tiles = units // kdim
    lead = (2 * tiles + 1) * kdim
    moves = [(w, mixer_ref.at[q]) for q, w in enumerate(mats)]
    moves += [(gate, flip_ref.at[0]), (up, flip_ref.at[1]), (down, ffn_buf.at[pl.ds(lead, units)])]
    moves = [pltpu.make_async_copy(x, y, sems.at[n]) for n, (x, y) in enumerate(moves)]
    for c in moves:
        c.start()
    for c in moves:
        c.wait()
    for q in range(2):
        for j in range(tiles):
            ffn_buf[pl.ds((q * tiles + j) * kdim, kdim), :] = flip_ref[q, pl.ds(j * kdim, kdim), :].T
    rest = pl.ds(tiles * kdim, units - tiles * kdim)
    ends = jnp.concatenate([flip_ref[0, rest, :], flip_ref[1, rest, :]], axis=0)
    ffn_buf[pl.ds(2 * tiles * kdim, kdim), :] = ends.T
    last = pltpu.make_async_copy(ffn_buf, ffn_ref, sems.at[len(moves)])
    last.start()
    last.wait()


def norm_body(*refs, n_blocks):
    blocks, gain_ref, xn_ref = refs[:n_blocks], refs[n_blocks], refs[n_blocks + 1]
    normalize(lax.axis_index("tp"), blocks, gain_ref, xn_ref)


def mixer_body(*refs, n_slots, channels, length):
    xn_ref, taps_ref = refs[:2]
    slots = refs[2 : 2 + n_slots]
    outs, o_ref = refs[2 + n_slots : -1], refs[-1]
    t = lax.axis_index("tp")
    i = lax.axis_index("fs")
    pairs = ring_offsets(n_slots)
    for slot, off in zip(slots, [o for pair in pairs for o in pair]):
        o_ref[(i + off) % n_slots] = slot[3]
    rows = 2 * length

    @pl.loop(0, xn_ref.shape[1] // rows)
    def _(r):
        sl = pl.ds(pl.multiple_of(r * rows, rows), rows)
        acc = None
        for n, (a, b) in enumerate(pairs):
            ka, kb = (i + a) % n_slots, (i + b) % n_slots
            wa, wb = slots[2 * n], slots[2 * n + 1]
            lhs = jnp.concatenate([xn_ref[ka, sl, :], xn_ref[kb, sl, :]], axis=1)
            rhs = jnp.concatenate(
                [jnp.concatenate([w[q] for q in range(3)], axis=1) for w in (wa, wb)], axis=0
            )
            part = jnp.dot(lhs, rhs, preferred_element_type=F32)
            acc = part if acc is None else acc + part
        acc = acc.astype(BF16).astype(F32)
        outer, inner, values = (acc[:, q * channels : (q + 1) * channels] for q in range(3))
        product = inner * values
        at = lax.broadcasted_iota(jnp.int32, product.shape, 0) % length
        tap_count = taps_ref.shape[0]
        conv = jnp.zeros(product.shape, F32)
        for q in range(tap_count):
            back = tap_count - 1 - q
            moved = product
            if back:
                moved = jnp.where(at >= back, pltpu.roll(product, back, 0), 0.0)
            lanes = pl.ds(pl.multiple_of(t * channels, channels), channels)
            conv = conv + taps_ref[pl.ds(q, 1), lanes] * moved
        gated = (outer * conv).astype(BF16)
        send_parts(t, gated, lambda k: o_ref[k], n_slots, outs, sl)


def send_parts(t, left, weight, n_slots, outs, sl):
    n = len(outs)
    per = n_slots // n
    for slot in range(n):
        b = block_of(t, slot, n)
        rhs = jnp.concatenate([weight(b * per + h) for h in range(per)], axis=1)
        outs[slot][sl, :] = jnp.dot(left, rhs, preferred_element_type=F32).astype(BF16)


def hidden_body(xn_ref, w_hbm, *refs, units):
    outs = refs[:-3]
    w_ref, acc_ref, sems = refs[-3:]
    t = lax.axis_index("tp")
    n_slots, _, lanes = w_ref.shape
    kdim = xn_ref.shape[2]
    tiles = units // lanes
    step = n_slots // 2

    def fetch(n):
        part = pl.ds(n * step, step)
        return pltpu.make_async_copy(w_hbm.at[part], w_ref.at[part], sems.at[n])

    fetch(0).start()
    acc_ref[...] = jnp.zeros(acc_ref.shape, F32)

    @pl.loop(0, 2)
    def _(n):
        fetch(n).wait()

        @pl.when(n == 0)
        def _():
            fetch(1).start()

        lhs = jnp.concatenate([xn_ref[n * step + h] for h in range(step)], axis=1)
        rhs = jnp.concatenate(
            [
                jnp.concatenate([w_ref[n * step + h, pl.ds(j * kdim, kdim), :] for j in range(2 * tiles + 1)], axis=1)
                for h in range(step)
            ],
            axis=0,
        )
        acc_ref[...] += jnp.dot(lhs, rhs, preferred_element_type=F32)

    full = tiles * lanes
    rest = units - full
    ends = acc_ref[:, 2 * full :]
    pieces = ((acc_ref[:, :full], acc_ref[:, full : 2 * full]), (ends[:, :rest], ends[:, rest:]))
    hidden = jnp.concatenate([(g / (1.0 + jnp.exp(-g)) * u).astype(BF16) for g, u in pieces], axis=1)
    down = pl.ds((2 * tiles + 1) * kdim, units)
    send_parts(t, hidden, lambda k: w_ref[k, down, :], n_slots, outs, slice(None))


def run_kernel(body, args, out_shape, scratch, name, flops, vmem=24, hbm=(), hbm_out=(), **static):
    def spec(far):
        return pl.BlockSpec(memory_space=pltpu.HBM if far else pltpu.VMEM)

    return pl.pallas_call(
        functools.partial(body, **static),
        out_shape=out_shape,
        in_specs=[spec(n in hbm) for n in range(len(args))],
        out_specs=[spec(n in hbm_out) for n in range(len(out_shape))],
        scratch_shapes=scratch,
        compiler_params=pltpu.CompilerParams(vmem_limit_bytes=vmem * 1024 * 1024),
        cost_estimate=pl.CostEstimate(flops=flops, transcendentals=0, bytes_accessed=1 << 20),
        name=name,
    )(*args)


def local(
    tokens,
    mix_gain,
    gate_outer,
    gate_inner,
    value_weight,
    conv_taps,
    mix_out,
    ffn_gain,
    ffn_gate,
    ffn_up,
    ffn_down,
    out_gain,
):
    seq_count, length, columns = tokens.shape
    row_count = seq_count * length
    n_tp = lax.axis_size("tp")
    n_fs = lax.axis_size("fs")
    width = columns * n_tp
    channels = gate_outer.shape[1]
    units = ffn_gate.shape[1]
    kdim = gate_outer.shape[0]
    mine = tokens.reshape(row_count, columns)
    order = [o for pair in ring_offsets(n_fs) for o in pair]

    mixer_w, ffn_w = run_kernel(
        pack_body,
        [gate_outer, gate_inner, value_weight, mix_out, ffn_gate.T, ffn_up.T, ffn_down],
        [
            jax.ShapeDtypeStruct((4, kdim, channels), BF16),
            jax.ShapeDtypeStruct((3 * units, kdim), BF16),
        ],
        [
            pltpu.VMEM((2, units, kdim), BF16),
            pltpu.VMEM((3 * units, kdim), BF16),
            pltpu.SemaphoreType.DMA((8,)),
        ],
        "pack",
        1 << 20,
        vmem=62,
        hbm=range(7),
        hbm_out=(1,),
    )
    ffn_all = lax.all_gather(ffn_w, "fs", axis=0, tiled=False)
    mixer_slots = ring(mixer_w, "fs")
    blocks = gather_rows(mine)

    part = jax.ShapeDtypeStruct((row_count, columns), BF16)
    xn = jax.ShapeDtypeStruct((n_fs, row_count, kdim), BF16)
    gains = (mix_gain.reshape(n_fs, kdim), ffn_gain.reshape(n_fs, kdim))
    (normed,) = run_kernel(norm_body, blocks + [gains[0]], [xn], [], "norm_mix", 1 << 30, n_blocks=n_tp)
    parts = run_kernel(
        mixer_body,
        [normed, conv_taps] + [mixer_slots[o] for o in order],
        [part] * n_tp,
        [pltpu.VMEM((n_fs, channels, kdim), BF16)],
        "mixer",
        2 * row_count * width * 4 * channels,
        n_slots=n_fs,
        channels=channels,
        length=length,
    )
    first = scatter_sum((parts[: n_tp // 2], parts[n_tp // 2 :]), mine).astype(BF16)
    blocks = gather_rows(first)
    (normed,) = run_kernel(norm_body, blocks + [gains[1]], [xn], [], "norm_ffn", 1 << 30, n_blocks=n_tp)
    parts = run_kernel(
        hidden_body,
        [normed, ffn_all],
        [part] * n_tp,
        [
            pltpu.VMEM(ffn_all.shape, BF16),
            pltpu.VMEM((row_count, 2 * units), F32),
            pltpu.SemaphoreType.DMA((2,)),
        ],
        "ffn",
        2 * row_count * width * 3 * units,
        vmem=52,
        hbm=(1,),
        units=units,
    )
    second = scatter_sum((parts[: n_tp // 2], parts[n_tp // 2 :]), first)
    squares = jnp.sum(second * second, axis=1)
    copies = jnp.broadcast_to(squares, (n_tp, row_count))
    squares = lax.all_to_all(copies, "tp", split_axis=0, concat_axis=0, tiled=True).sum(axis=0)
    factor = lax.rsqrt(squares.reshape(row_count) / width + 1e-06)
    own_gain = lax.dynamic_slice_in_dim(out_gain, lax.axis_index("tp") * columns, columns, 0)
    result = second * factor[:, None] * own_gain
    return result.astype(BF16).reshape(seq_count, length, columns)


def solution(mesh):
    in_specs = (
        P(("grp", "fs"), None, "tp"),
        P(),
        P("fs", "tp"),
        P("fs", "tp"),
        P("fs", "tp"),
        P(),
        P("tp", "fs"),
        P(),
        P("fs", "tp"),
        P("fs", "tp"),
        P("tp", "fs"),
        P(),
    )
    out_specs = P(("grp", "fs"), None, "tp")
    return jax.shard_map(local, mesh=mesh, in_specs=in_specs, out_specs=out_specs, check_vma=False)
```
